32 devices in a mesh: fs: 16 (over z, y, x), tp: 2 (over core).
Axes of the slice: x: 2, y: 2, z: 4, core: 2. Of those that a mesh axis runs over, the one named last changes fastest.
Arguments:
- normed_input: bfloat16 [8192, 2048], P('fs', 'tp'), may hold values from -6 to 6
- cotangent: bfloat16 [8192, 2048], P('fs', 'tp'), may hold values from -6 to 6
- up_weight: bfloat16 [2048, 8192], P('fs', 'tp'), may hold values from -0.125 to 0.125
- down_weight: bfloat16 [8192, 2048], P('tp', 'fs'), may hold values from -0.0625 to 0.0625
Outputs:
- input_grad: bfloat16 [8192, 2048], P('fs', 'tp')
- up_grad: float32 [2048, 8192], P('fs', 'tp')
- down_grad: float32 [8192, 2048], P('tp', 'fs')
The draws below stay inside these ranges and needn't reach their ends.
All inputs are finite; a program needn't handle non-finite values.
Results may differ from the reference program's by a relative error of at most 0.018.
Values may be sent and summed in bfloat16 or wider, within the bound.
No kernel may reach another device: no remote copies, remote signals or barrier semaphores. Data moves between devices by JAX's collectives and lax.ppermute only.
A program may use at most 192 MiB of HBM per device.

```python
import jax
import jax.numpy as jnp
from jax import lax

D = 2048
FF = 8192
TOKENS = 8192
FF_BLOCKS = 2


def strengthened(array, key, source, target, blocks, factor):
    owner, partner = [(jnp.arange(array.shape[axis_at]) // (array.shape[axis_at] // blocks)).reshape([-1 if axis == axis_at else 1 for axis in range(array.ndim)]) for axis_at in (source, target)]
    chosen = jax.random.permutation(key, blocks)[partner]
    strong = (owner == chosen) | (owner == (partner + blocks // 2) % blocks)
    return jnp.where(strong, factor * array, array)


def steps_of(stream_key, extent, shards, smallest, top_value):
    gain = 1.0
    for position, shards_of in shards:
        steps = jax.random.uniform(jax.random.fold_in(jax.random.fold_in(stream_key, 6), position), (shards_of,), jnp.float32, smallest / len(shards), top_value / len(shards))
        gain = gain * jnp.repeat(jnp.exp(steps), extent[position] // shards_of).reshape((-1,) + (1,) * (len(extent) - 1 - position))
    return gain


def bell_draw(stream_key, dims, spread, limit, pieces=(), kind=jnp.bfloat16):
    array = spread * jax.random.normal(stream_key, dims, jnp.float32)
    if pieces:
        array = array * steps_of(stream_key, dims, pieces, -0.22, 0.18)
    return jnp.clip(array, -limit, limit).astype(kind)


def heavy_noise(own_key, extent, spread, limit, cuts, heavy, kind=jnp.bfloat16):
    result = spread * jax.random.normal(own_key, extent, jnp.float32)
    if cuts:
        result = result * steps_of(own_key, extent, cuts, -0.22, 0.18)
    return jnp.clip(strengthened(result, jax.random.fold_in(own_key, 3), *heavy), -limit, limit).astype(kind)


def setup_inputs(seed: int = 0) -> dict:
    splits = jax.random.split(jax.random.key(seed), 5)
    normed_input = heavy_noise(splits[0], (TOKENS, D), 1.0, 6.0, ((0, 16), (1, 2)), (0, 1, 16, 2.0))
    cotangent = heavy_noise(splits[1], (TOKENS, D), 1.0, 6.0, ((0, 16), (1, 2)), (0, 1, 16, 2.0))
    up_weight = bell_draw(splits[2], (D, FF), D ** -0.5, 0.125, ((0, 16), (1, 2)))
    down_weight = bell_draw(splits[3], (FF, D), FF ** -0.5, 0.0625, ((0, 2), (1, 16)))
    return {"normed_input": normed_input, "cotangent": cotangent, "up_weight": up_weight, "down_weight": down_weight}


def reference(normed_input, cotangent, up_weight, down_weight):
    tokens = normed_input.shape[0]
    width = FF // FF_BLOCKS
    scale = lax.rsqrt(jnp.asarray(tokens, jnp.float32))

    def block(total, index):
        start = (index * width).astype(jnp.int32)
        up_block = lax.dynamic_slice_in_dim(up_weight, start, width, 1)
        down_block = lax.dynamic_slice_in_dim(down_weight, start, width, 0)
        pre = jnp.dot(normed_input, up_block, preferred_element_type=jnp.float32)
        rectified = jax.nn.relu(pre)
        act = (rectified * rectified).astype(jnp.bfloat16)
        act_grad = jnp.dot(cotangent, down_block.T, preferred_element_type=jnp.float32)
        pre_grad = (2.0 * rectified * act_grad).astype(jnp.bfloat16)
        down_part = jnp.dot(act.T, cotangent, preferred_element_type=jnp.float32) * scale
        up_part = jnp.dot(normed_input.T, pre_grad, preferred_element_type=jnp.float32) * scale
        partial_value = jnp.dot(pre_grad, up_block.T, preferred_element_type=jnp.float32).astype(jnp.bfloat16)
        partial_value = lax.optimization_barrier(partial_value)
        return (total + partial_value.astype(jnp.float32), (up_part, down_part))
    start_total = jnp.zeros(normed_input.shape, jnp.float32)
    total, parts = lax.scan(block, start_total, jnp.arange(FF_BLOCKS, dtype=jnp.int32))
    up_parts, down_parts = parts
    up_grad = jnp.moveaxis(up_parts, 0, 1).reshape(D, FF)
    down_grad = down_parts.reshape(FF, D)
    return (total.astype(jnp.bfloat16), up_grad, down_grad)
```

```python
import jax
import jax.numpy as jnp
from jax import lax
from jax.sharding import PartitionSpec as P

AXES = ("fs", "tp")
CHUNKS = 1
BF, F32 = jnp.bfloat16, jnp.float32


def dot(left, right, dims):
    return lax.dot_general(left, right, (dims, ((), ())), preferred_element_type=F32)


def place(buffer, piece, axis, index):
    return lax.dynamic_update_slice_in_dim(buffer, jnp.expand_dims(piece, axis), index, axis)


def pick(array, axis, index):
    return lax.dynamic_index_in_dim(array, index, axis, keepdims=False)


def per_device(x, dy, up, down):
    n, m = lax.axis_size("fs"), lax.axis_size("tp")
    f, t = lax.axis_index("fs"), lax.axis_index("tp")
    rows, part = x.shape
    d_rows, ff = up.shape
    planes = n // 4
    px, py, pz = f % 2, (f // 2) % 2, f // 4
    scale = lax.rsqrt(jnp.asarray(rows * n, F32))
    turn = t * (planes // m) if planes >= m else 0

    def send(value, mask, core=0):
        perm = [(i * m + c, (i ^ mask) * m + (c ^ core)) for i in range(n) for c in range(m)]
        return lax.ppermute(value, AXES, perm)

    def tokens(value):
        near = send(value, 4)
        pieces = [value, send(value, 2), near, send(near, 2)]
        return jnp.concatenate(
            [jnp.concatenate([p] + [send(p, 0, c) for c in range(1, m)], axis=1) for p in pieces]
        )

    block = ff // 4
    width = block // CHUNKS

    def at(z):
        return z ^ turn

    def weights(w, chunk, rowwise):
        if rowwise:
            w = w.reshape(d_rows, 2, 2, CHUNKS, width)[:, :, :, chunk]
        else:
            w = w.reshape(2, 2, CHUNKS, width, d_rows)[:, :, chunk]
        ax = 1 if rowwise else 0
        mine, theirs = pick(w, ax, py), send(pick(w, ax, 1 - py), 2)
        both = place(place(jnp.zeros((2,) + mine.shape, BF), mine, 0, py), theirs, 0, 1 - py)
        zl = pz % 2
        got = {}
        halves = {b: pick(both, ax + 1, zl ^ b) for b in (0, 1)}
        for mask in range(planes):
            piece = halves[mask % 2]
            got[mask] = send(piece, 4 * mask) if mask else piece
        whole = jnp.zeros((planes,) + halves[0].shape, BF)
        for mask in range(planes):
            whole = place(whole, got[mask], 0, at(pz ^ mask))
        other = send(whole, 1)
        full = jnp.zeros((planes, 2, 2) + whole.shape[2:], BF)
        full = place(place(full, whole, 2, px), other, 2, 1 - px)
        if rowwise:
            return full.reshape(n * d_rows, width)
        return full.transpose(3, 0, 1, 2, 4).reshape(width, n * d_rows)

    def reduce_out(g, rowwise):
        g = (g * scale).astype(BF)
        if rowwise:
            g = g.reshape(planes, 2, 2, d_rows, width)
        else:
            g = g.reshape(width, planes, 2, 2, d_rows).transpose(1, 2, 3, 0, 4)
        mine, theirs = pick(g, 2, px), pick(g, 2, 1 - px)
        h = (mine.astype(F32) + send(theirs, 1).astype(F32)).astype(BF)
        total = [pick(h, 0, at(pz)).astype(F32), None]
        for mask in range(1, planes):
            got = send(pick(h, 0, at(pz ^ mask)), 4 * mask).astype(F32)
            b = mask % 2
            total[b] = got if total[b] is None else total[b] + got
        out = jnp.stack(total)
        mine, theirs = pick(out, 1, py), pick(out, 1, 1 - py)
        other = send(theirs.astype(BF), 2).astype(F32)
        return mine, other

    x4, dy4 = tokens(x), tokens(dy)
    zl = pz % 2
    dx = None
    ups, downs = [], []
    for chunk in range(CHUNKS):
        wu = weights(up, chunk, True)
        wd = weights(down, chunk, False)
        rect = jax.nn.relu(dot(x4, wu, ((1,), (0,))))
        act = (rect * rect).astype(BF)
        pre_grad = (2.0 * rect * dot(dy4, wd, ((1,), (1,)))).astype(BF)
        downs.append(reduce_out(dot(act, dy4, ((0,), (0,))), False))
        ups.append(reduce_out(dot(x4, pre_grad, ((0,), (0,))), True))
        term = dot(pre_grad, wu, ((1,), (1,)))
        dx = term if dx is None else dx + term

    dx = dx.astype(BF).reshape(4, rows, m, part)
    own = dx[:, :, 0].astype(F32)
    for c in range(1, m):
        own = own + send(dx[:, :, c], 0, c).astype(F32)
    near = own[0::2] + send(own[1::2].astype(BF), 2).astype(F32)
    input_grad = (near[0] + send(near[1].astype(BF), 4).astype(F32)).astype(BF)

    def join(parts, rowwise):
        out = jnp.zeros((2, 2, CHUNKS) + parts[0][0].shape[1:], F32)
        for chunk, (mine, other) in enumerate(parts):
            for value, y in ((mine, py), (other, 1 - py)):
                for b in (0, 1):
                    start = (y, zl ^ b, chunk) + (0,) * (out.ndim - 3)
                    out = lax.dynamic_update_slice(out, value[b][None, None, None], start)
        if rowwise:
            return out.transpose(3, 0, 1, 2, 4).reshape(d_rows, ff)
        return out.reshape(ff, d_rows)

    return input_grad, join(ups, True), join(downs, False)


def solution(mesh):
    in_specs = (P("fs", "tp"), P("fs", "tp"), P("fs", "tp"), P("tp", "fs"))
    out_specs = (P("fs", "tp"), P("fs", "tp"), P("tp", "fs"))
    return jax.shard_map(
        per_device, mesh=mesh, in_specs=in_specs, out_specs=out_specs, check_vma=False
    )
```

```python
import functools

import jax
import jax.numpy as jnp
from jax import lax
from jax.experimental import pallas as pl
from jax.experimental.pallas import tpu as pltpu
from jax.sharding import PartitionSpec as P


AXES = ("fs", "tp")
CHUNKS = 1
BF, F32 = jnp.bfloat16, jnp.float32


def dot(left, right, dims):
    return lax.dot_general(left, right, (dims, ((), ())), preferred_element_type=F32)


def place(buffer, piece, axis, index):
    return lax.dynamic_update_slice_in_dim(buffer, jnp.expand_dims(piece, axis), index, axis)


def pick(array, axis, index):
    return lax.dynamic_index_in_dim(array, index, axis, keepdims=False)


def plain(x, dy, up, down):
    n, m = lax.axis_size("fs"), lax.axis_size("tp")
    f, t = lax.axis_index("fs"), lax.axis_index("tp")
    rows, part = x.shape
    d_rows, ff = up.shape
    planes = n // 4
    px, py, pz = f % 2, (f // 2) % 2, f // 4
    scale = lax.rsqrt(jnp.asarray(rows * n, F32))
    turn = t * (planes // m) if planes >= m else 0

    def send(value, mask, core=0):
        perm = [(i * m + c, (i ^ mask) * m + (c ^ core)) for i in range(n) for c in range(m)]
        return lax.ppermute(value, AXES, perm)

    def tokens(value):
        near = send(value, 4)
        pieces = [value, send(value, 2), near, send(near, 2)]
        return jnp.concatenate(
            [jnp.concatenate([p] + [send(p, 0, c) for c in range(1, m)], axis=1) for p in pieces]
        )

    block = ff // 4
    width = block // CHUNKS

    def at(z):
        return z ^ turn

    def weights(w, chunk, rowwise):
        if rowwise:
            w = w.reshape(d_rows, 2, 2, CHUNKS, width)[:, :, :, chunk]
        else:
            w = w.reshape(2, 2, CHUNKS, width, d_rows)[:, :, chunk]
        ax = 1 if rowwise else 0
        mine, theirs = pick(w, ax, py), send(pick(w, ax, 1 - py), 2)
        both = place(place(jnp.zeros((2,) + mine.shape, BF), mine, 0, py), theirs, 0, 1 - py)
        zl = pz % 2
        got = {}
        halves = {b: pick(both, ax + 1, zl ^ b) for b in (0, 1)}
        for mask in range(planes):
            piece = halves[mask % 2]
            got[mask] = send(piece, 4 * mask) if mask else piece
        whole = jnp.zeros((planes,) + halves[0].shape, BF)
        for mask in range(planes):
            whole = place(whole, got[mask], 0, at(pz ^ mask))
        other = send(whole, 1)
        full = jnp.zeros((planes, 2, 2) + whole.shape[2:], BF)
        full = place(place(full, whole, 2, px), other, 2, 1 - px)
        if rowwise:
            return full.reshape(n * d_rows, width)
        return full.transpose(3, 0, 1, 2, 4).reshape(width, n * d_rows)

    def reduce_out(g, rowwise):
        g = (g * scale).astype(BF)
        if rowwise:
            g = g.reshape(planes, 2, 2, d_rows, width)
        else:
            g = g.reshape(width, planes, 2, 2, d_rows).transpose(1, 2, 3, 0, 4)
        mine, theirs = pick(g, 2, px), pick(g, 2, 1 - px)
        h = (mine.astype(F32) + send(theirs, 1).astype(F32)).astype(BF)
        total = [pick(h, 0, at(pz)).astype(F32), None]
        for mask in range(1, planes):
            got = send(pick(h, 0, at(pz ^ mask)), 4 * mask).astype(F32)
            b = mask % 2
            total[b] = got if total[b] is None else total[b] + got
        out = jnp.stack(total)
        mine, theirs = pick(out, 1, py), pick(out, 1, 1 - py)
        other = send(theirs.astype(BF), 2).astype(F32)
        return mine, other

    x4, dy4 = tokens(x), tokens(dy)
    zl = pz % 2
    dx = None
    ups, downs = [], []
    for chunk in range(CHUNKS):
        wu = weights(up, chunk, True)
        wd = weights(down, chunk, False)
        rect = jax.nn.relu(dot(x4, wu, ((1,), (0,))))
        act = (rect * rect).astype(BF)
        pre_grad = (2.0 * rect * dot(dy4, wd, ((1,), (1,)))).astype(BF)
        downs.append(reduce_out(dot(act, dy4, ((0,), (0,))), False))
        ups.append(reduce_out(dot(x4, pre_grad, ((0,), (0,))), True))
        term = dot(pre_grad, wu, ((1,), (1,)))
        dx = term if dx is None else dx + term

    dx = dx.astype(BF).reshape(4, rows, m, part)
    own = dx[:, :, 0].astype(F32)
    for c in range(1, m):
        own = own + send(dx[:, :, c], 0, c).astype(F32)
    near = own[0::2] + send(own[1::2].astype(BF), 2).astype(F32)
    input_grad = (near[0] + send(near[1].astype(BF), 4).astype(F32)).astype(BF)

    def join(parts, rowwise):
        out = jnp.zeros((2, 2, CHUNKS) + parts[0][0].shape[1:], F32)
        for chunk, (mine, other) in enumerate(parts):
            for value, y in ((mine, py), (other, 1 - py)):
                for b in (0, 1):
                    start = (y, zl ^ b, chunk) + (0,) * (out.ndim - 3)
                    out = lax.dynamic_update_slice(out, value[b][None, None, None], start)
        if rowwise:
            return out.transpose(3, 0, 1, 2, 4).reshape(d_rows, ff)
        return out.reshape(ff, d_rows)

    return input_grad, join(ups, True), join(downs, False)


LANES = 128
NT, NN, TN = ((1,), (1,)), ((1,), (0,)), ((0,), (0,))


def call(body, outs, scratch, sems, flops, args):
    nbytes = sum(a.size * a.dtype.itemsize for a in args) + sum(
        2 * functools.reduce(lambda p, q: p * q, o) for o in outs
    )
    return pl.pallas_call(
        body,
        out_shape=[jax.ShapeDtypeStruct(o, BF) for o in outs],
        in_specs=[pl.BlockSpec(memory_space=pltpu.SMEM)]
        + [pl.BlockSpec(memory_space=pl.ANY)] * (len(args) - 1),
        out_specs=[pl.BlockSpec(memory_space=pl.ANY)] * len(outs),
        scratch_shapes=[pltpu.VMEM(s, BF) for s in scratch]
        + [pltpu.SemaphoreType.DMA(s if isinstance(s, tuple) else (s,)) for s in sems],
        cost_estimate=pl.CostEstimate(flops=flops, bytes_accessed=nbytes, transcendentals=0),
        compiler_params=pltpu.CompilerParams(vmem_limit_bytes=26 * 2**20),
    )(*args)


def start(copies):
    for copy in copies:
        copy.start()
    return copies


def wait(copies):
    for copy in copies:
        copy.wait()


def weight_copies(base, pieces, dest, sem):
    copies = []
    for mz, row in enumerate(pieces):
        for kx, piece in enumerate(row):
            for ky in range(2):
                pos = pl.multiple_of((base ^ (mz * 4 + ky * 2 + kx)) * LANES, LANES)
                copies.append(
                    pltpu.make_async_copy(
                        piece.at[ky], dest.at[:, pl.ds(pos, LANES)], sem.at[len(copies)]
                    )
                )
    return copies


def token_copies(pieces, dest, sem):
    m = len(pieces[0])
    rows, part = pieces[0][0].shape
    return [
        [
            pltpu.make_async_copy(
                piece,
                dest.at[pl.ds(p * rows, rows), pl.ds(c * part, part)],
                sem.at[p * m + c],
            )
            for c, piece in enumerate(row)
        ]
        for p, row in enumerate(pieces)
    ]


def group(refs, count, size):
    return [refs[i * size : (i + 1) * size] for i in range(count)]


def hidden_kernel(planes, m, second, base_ref, *refs):
    tokens, refs = group(refs, 4, m), refs[4 * m :]
    weights, refs = group(refs, planes, 2), refs[2 * planes :]
    if second:
        rect, out, wv, tv, rv, ov, wsem, tsem, rsem, osem = refs
        outs = [(out, ov)]
    else:
        act, rect, wv, tv, rv, ov, wsem, tsem, osem = refs
        outs = [(act, ov), (rect, rv)]
    rows = tokens[0][0].shape[0]
    width = wv.shape[0]
    wcopies = start(weight_copies(base_ref[0], weights, wv, wsem))
    tcopies = token_copies(tokens, tv, tsem)
    for row in tcopies:
        start(row)
    if second:
        rcopies = start([pltpu.make_async_copy(rect.at[p], rv.at[p], rsem.at[p]) for p in range(4)])
    wait(wcopies)
    tile = min(width, 256)
    ocopies = []
    for p in range(4):
        wait(tcopies[p])
        if second:
            rcopies[p].wait()

        @pl.loop(0, width // tile)
        def _(i):
            at = pl.ds(pl.multiple_of(i * tile, tile), tile)
            o = dot(wv[at, :], tv[pl.ds(p * rows, rows), :], NT)
            if second:
                ov[p, at, :] = (2.0 * rv[p, at, :].astype(F32) * o).astype(BF)
            else:
                r = jnp.maximum(o, 0.0)
                rv[p, at, :] = r.astype(BF)
                ov[p, at, :] = (r * r).astype(BF)

        for k, (dest, source) in enumerate(outs):
            ocopies += start(
                [pltpu.make_async_copy(source.at[p], dest.at[p], osem.at[p * len(outs) + k])]
            )
    wait(ocopies)


def grad_kernel(planes, m, scale, base_ref, *refs):
    tokens, refs = group(refs, 4, m), refs[4 * m :]
    hidden, *outs, av, tv, ov, tsem, asem, osem = refs
    rows = tokens[0][0].shape[0]
    width = av.shape[0]
    base = base_ref[0]
    acopies = start(
        [
            pltpu.make_async_copy(hidden.at[p], av.at[:, pl.ds(p * rows, rows)], asem.at[p])
            for p in range(4)
        ]
    )
    tcopies = token_copies(tokens, tv, tsem)
    for c in range(m):
        start([row[c] for row in tcopies])
    wait(acopies)
    tile = min(width, 512)
    even = (base & 1) == 0
    each = 2 * planes // m

    def out_copies(mz, ky):
        return [
            pltpu.make_async_copy(
                ov.at[mz, k, ky], outs[2 * mz + k].at[ky], osem.at[mz, k, ky]
            )
            for k in range(2)
        ]

    for c in range(m):
        wait([row[c] for row in tcopies])

        @pl.loop(c * each, (c + 1) * each)
        def _(q):
            mask = (base >> 1) ^ q
            mz, ky = mask >> 1, mask & 1
            cols = pl.ds(pl.multiple_of(q * 2 * LANES, 2 * LANES), 2 * LANES)

            @pl.loop(0, width // tile)
            def _(i):
                at = pl.ds(pl.multiple_of(i * tile, tile), tile)
                o = dot(av[at, :], tv[:, cols], NN) * scale
                lo, hi = o[:, :LANES], o[:, LANES:]
                ov[mz, 0, ky, at, :] = jnp.where(even, lo, hi).astype(BF)
                ov[mz, 1, ky, at, :] = jnp.where(even, hi, lo).astype(BF)

            for plane in range(planes):

                @pl.when(mz == plane)
                def _():
                    start(out_copies(plane, ky))

    for plane in range(planes):
        for ky in range(2):
            wait(out_copies(plane, ky))


def input_kernel(planes, m, base_ref, *refs):
    hidden, refs = refs[0], refs[1:]
    weights, refs = group(refs, planes, 2), refs[2 * planes :]
    outs, (wv, av, ov, wsem, asem, osem) = refs[: 4 * m], refs[4 * m :]
    part = outs[0].shape[1]
    wcopies = start(weight_copies(base_ref[0], weights, wv, wsem))
    acopies = start([pltpu.make_async_copy(hidden.at[p], av.at[p], asem.at[p]) for p in range(4)])
    wait(wcopies)
    wait(acopies)
    ocopies = []
    for c in range(m - 1, -1, -1):
        for p in range(3, -1, -1):
            ov[c, p] = dot(av[p], wv[:, c * part : (c + 1) * part], TN).astype(BF)
            k = c * 4 + p
            ocopies += start([pltpu.make_async_copy(ov.at[c, p], outs[k], osem.at[k])])
    wait(ocopies)


def per_device(x, dy, up, down):
    n, m = lax.axis_size("fs"), lax.axis_size("tp")
    rows, part = x.shape
    d_rows, ff = up.shape
    planes = n // 4
    if d_rows != LANES or planes < m:
        return plain(x, dy, up, down)
    f, t = lax.axis_index("fs"), lax.axis_index("tp")
    py, zl = (f // 2) % 2, (f // 4) % 2
    base = (f ^ (4 * t * (planes // m))).astype(jnp.int32).reshape(1)
    width = ff // 4
    scale = float(rows * n) ** -0.5
    flops = 2 * 4 * rows * width * n * d_rows

    def send(value, mask, core=0):
        perm = [(i * m + c, (i ^ mask) * m + (c ^ core)) for i in range(n) for c in range(m)]
        return lax.ppermute(value, AXES, perm)

    def gather_tokens(value):
        near = send(value, 4)
        side = send(value, 2)
        pieces = (value, side, near, send(near, 2))
        return [[p] + [send(p, 0, c) for c in range(1, m)] for p in pieces]

    def gather_weights(w):
        w = w.reshape(2, 2, width, d_rows)
        mine, theirs = pick(w, 0, py), send(pick(w, 0, 1 - py), 2)
        both = jnp.stack([mine, theirs])
        halves = [pick(both, 1, zl), pick(both, 1, 1 - zl)]
        pieces = []
        for mz in range(planes):
            piece = send(halves[mz % 2], 4 * mz) if mz else halves[0]
            pieces.append([piece, send(piece, 1)])
        return pieces

    def flat(lists):
        return [a for row in lists for a in row]

    x4 = gather_tokens(x)
    wu = gather_weights(up.T)
    dy4 = gather_tokens(dy)
    wd = gather_weights(down)
    every = 4 * rows
    hid, feats = (4, width, rows), n * d_rows
    nw, nt = 4 * planes, 4 * m

    act, rect = call(
        functools.partial(hidden_kernel, planes, m, False),
        [hid, hid],
        [(width, feats), (every, feats), hid, hid],
        [nw, nt, 8],
        flops,
        [base, *flat(x4), *flat(wu)],
    )

    def grad(tokens, hidden):
        return call(
            functools.partial(grad_kernel, planes, m, scale),
            [(2, width, LANES)] * (2 * planes),
            [(width, every), (every, feats), (planes, 2, 2, width, LANES)],
            [nt, 4, (planes, 2, 2)],
            flops,
            [base, *flat(tokens), hidden],
        )

    def scatter(parts):
        total = [None, None]
        for mz in reversed(range(planes)):
            got = send(parts[2 * mz + 1], 1).astype(F32)
            value = parts[2 * mz].astype(F32) + got
            if mz:
                value = value.astype(BF)
            if mz:
                value = send(value, 4 * mz).astype(F32)
            b = mz % 2
            total[b] = value if total[b] is None else total[b] + value
        other = send(jnp.stack([total[0][1], total[1][1]]).astype(BF), 2)
        a, b = total[0][0], total[1][0]
        c, d = other[0].astype(F32), other[1].astype(F32)
        a, b = jnp.where(zl == 0, a, b), jnp.where(zl == 0, b, a)
        c, d = jnp.where(zl == 0, c, d), jnp.where(zl == 0, d, c)
        a, b, c, d = (
            jnp.where(py == 0, a, c),
            jnp.where(py == 0, b, d),
            jnp.where(py == 0, c, a),
            jnp.where(py == 0, d, b),
        )
        return jnp.concatenate([a, b, c, d])

    down_grad = scatter(grad(dy4, act))
    (pre_grad,) = call(
        functools.partial(hidden_kernel, planes, m, True),
        [hid],
        [(width, feats), (every, feats), hid, hid],
        [nw, nt, 4, 4],
        flops,
        [base, *flat(dy4), *flat(wd), rect],
    )
    up_grad = scatter(grad(x4, pre_grad)).T
    dx = call(
        functools.partial(input_kernel, planes, m),
        [(rows, part)] * (4 * m),
        [(width, feats), hid, (m, 4, rows, part)],
        [nw, 4, 4 * m],
        flops,
        [base, pre_grad, *flat(wu)],
    )
    own = [None] * 4
    for p in range(3, -1, -1):
        own[p] = dx[p].astype(F32)
        for c in range(1, m):
            own[p] = own[p] + send(dx[4 * c + p], 0, c).astype(F32)
    far = own[2] + send(own[3].astype(BF), 2).astype(F32)
    near = own[0] + send(own[1].astype(BF), 2).astype(F32)
    input_grad = (near + send(far.astype(BF), 4).astype(F32)).astype(BF)
    return input_grad, up_grad, down_grad


def solution(mesh):
    in_specs = (P("fs", "tp"), P("fs", "tp"), P("fs", "tp"), P("tp", "fs"))
    out_specs = (P("fs", "tp"), P("fs", "tp"), P("tp", "fs"))

    return jax.shard_map(
        per_device, mesh=mesh, in_specs=in_specs, out_specs=out_specs, check_vma=False
    )
```

```python
import functools

import jax
import jax.numpy as jnp
from jax import lax
from jax.experimental import pallas as pl
from jax.experimental.pallas import tpu as pltpu
from jax.sharding import PartitionSpec as P


AXES = ("fs", "tp")
CHUNKS = 1
BF, F32 = jnp.bfloat16, jnp.float32


def dot(left, right, dims):
    return lax.dot_general(left, right, (dims, ((), ())), preferred_element_type=F32)


def place(buffer, piece, axis, index):
    return lax.dynamic_update_slice_in_dim(buffer, jnp.expand_dims(piece, axis), index, axis)


def pick(array, axis, index):
    return lax.dynamic_index_in_dim(array, index, axis, keepdims=False)


def plain(x, dy, up, down):
    n, m = lax.axis_size("fs"), lax.axis_size("tp")
    f, t = lax.axis_index("fs"), lax.axis_index("tp")
    rows, part = x.shape
    d_rows, ff = up.shape
    planes = n // 4
    px, py, pz = f % 2, (f // 2) % 2, f // 4
    scale = lax.rsqrt(jnp.asarray(rows * n, F32))
    turn = t * (planes // m) if planes >= m else 0

    def send(value, mask, core=0):
        perm = [(i * m + c, (i ^ mask) * m + (c ^ core)) for i in range(n) for c in range(m)]
        return lax.ppermute(value, AXES, perm)

    def tokens(value):
        near = send(value, 4)
        pieces = [value, send(value, 2), near, send(near, 2)]
        return jnp.concatenate(
            [jnp.concatenate([p] + [send(p, 0, c) for c in range(1, m)], axis=1) for p in pieces]
        )

    block = ff // 4
    width = block // CHUNKS

    def at(z):
        return z ^ turn

    def weights(w, chunk, rowwise):
        if rowwise:
            w = w.reshape(d_rows, 2, 2, CHUNKS, width)[:, :, :, chunk]
        else:
            w = w.reshape(2, 2, CHUNKS, width, d_rows)[:, :, chunk]
        ax = 1 if rowwise else 0
        mine, theirs = pick(w, ax, py), send(pick(w, ax, 1 - py), 2)
        both = place(place(jnp.zeros((2,) + mine.shape, BF), mine, 0, py), theirs, 0, 1 - py)
        zl = pz % 2
        got = {}
        halves = {b: pick(both, ax + 1, zl ^ b) for b in (0, 1)}
        for mask in range(planes):
            piece = halves[mask % 2]
            got[mask] = send(piece, 4 * mask) if mask else piece
        whole = jnp.zeros((planes,) + halves[0].shape, BF)
        for mask in range(planes):
            whole = place(whole, got[mask], 0, at(pz ^ mask))
        other = send(whole, 1)
        full = jnp.zeros((planes, 2, 2) + whole.shape[2:], BF)
        full = place(place(full, whole, 2, px), other, 2, 1 - px)
        if rowwise:
            return full.reshape(n * d_rows, width)
        return full.transpose(3, 0, 1, 2, 4).reshape(width, n * d_rows)

    def reduce_out(g, rowwise):
        g = (g * scale).astype(BF)
        if rowwise:
            g = g.reshape(planes, 2, 2, d_rows, width)
        else:
            g = g.reshape(width, planes, 2, 2, d_rows).transpose(1, 2, 3, 0, 4)
        mine, theirs = pick(g, 2, px), pick(g, 2, 1 - px)
        h = (mine.astype(F32) + send(theirs, 1).astype(F32)).astype(BF)
        total = [pick(h, 0, at(pz)).astype(F32), None]
        for mask in range(1, planes):
            got = send(pick(h, 0, at(pz ^ mask)), 4 * mask).astype(F32)
            b = mask % 2
            total[b] = got if total[b] is None else total[b] + got
        out = jnp.stack(total)
        mine, theirs = pick(out, 1, py), pick(out, 1, 1 - py)
        other = send(theirs.astype(BF), 2).astype(F32)
        return mine, other

    x4, dy4 = tokens(x), tokens(dy)
    zl = pz % 2
    dx = None
    ups, downs = [], []
    for chunk in range(CHUNKS):
        wu = weights(up, chunk, True)
        wd = weights(down, chunk, False)
        rect = jax.nn.relu(dot(x4, wu, ((1,), (0,))))
        act = (rect * rect).astype(BF)
        pre_grad = (2.0 * rect * dot(dy4, wd, ((1,), (1,)))).astype(BF)
        downs.append(reduce_out(dot(act, dy4, ((0,), (0,))), False))
        ups.append(reduce_out(dot(x4, pre_grad, ((0,), (0,))), True))
        term = dot(pre_grad, wu, ((1,), (1,)))
        dx = term if dx is None else dx + term

    dx = dx.astype(BF).reshape(4, rows, m, part)
    own = dx[:, :, 0].astype(F32)
    for c in range(1, m):
        own = own + send(dx[:, :, c], 0, c).astype(F32)
    near = own[0::2] + send(own[1::2].astype(BF), 2).astype(F32)
    input_grad = (near[0] + send(near[1].astype(BF), 4).astype(F32)).astype(BF)

    def join(parts, rowwise):
        out = jnp.zeros((2, 2, CHUNKS) + parts[0][0].shape[1:], F32)
        for chunk, (mine, other) in enumerate(parts):
            for value, y in ((mine, py), (other, 1 - py)):
                for b in (0, 1):
                    start = (y, zl ^ b, chunk) + (0,) * (out.ndim - 3)
                    out = lax.dynamic_update_slice(out, value[b][None, None, None], start)
        if rowwise:
            return out.transpose(3, 0, 1, 2, 4).reshape(d_rows, ff)
        return out.reshape(ff, d_rows)

    return input_grad, join(ups, True), join(downs, False)


LANES = 128
NT, NN, TN = ((1,), (1,)), ((1,), (0,)), ((0,), (0,))


def call(body, outs, scratch, sems, flops, args):
    nbytes = sum(a.size * a.dtype.itemsize for a in args) + sum(
        2 * functools.reduce(lambda p, q: p * q, o) for o in outs
    )
    return pl.pallas_call(
        body,
        out_shape=[jax.ShapeDtypeStruct(o, BF) for o in outs],
        in_specs=[pl.BlockSpec(memory_space=pltpu.SMEM)]
        + [pl.BlockSpec(memory_space=pl.ANY)] * (len(args) - 1),
        out_specs=[pl.BlockSpec(memory_space=pl.ANY)] * len(outs),
        scratch_shapes=[pltpu.VMEM(s, BF) for s in scratch]
        + [pltpu.SemaphoreType.DMA(s if isinstance(s, tuple) else (s,)) for s in sems],
        cost_estimate=pl.CostEstimate(flops=flops, bytes_accessed=nbytes, transcendentals=0),
        compiler_params=pltpu.CompilerParams(vmem_limit_bytes=26 * 2**20),
    )(*args)


def start(copies):
    for copy in copies:
        copy.start()
    return copies


def wait(copies):
    for copy in copies:
        copy.wait()


def weight_copies(base, pieces, dest, sem):
    copies = []
    for mz, row in enumerate(pieces):
        for kx, piece in enumerate(row):
            for ky in range(2):
                pos = pl.multiple_of((base ^ (mz * 4 + ky * 2 + kx)) * LANES, LANES)
                copies.append(
                    pltpu.make_async_copy(
                        piece.at[ky], dest.at[:, pl.ds(pos, LANES)], sem.at[len(copies)]
                    )
                )
    return copies


def token_copies(pieces, dest, sem):
    m = len(pieces[0])
    rows, part = pieces[0][0].shape
    return [
        [
            pltpu.make_async_copy(
                piece,
                dest.at[pl.ds(p * rows, rows), pl.ds(c * part, part)],
                sem.at[p * m + c],
            )
            for c, piece in enumerate(row)
        ]
        for p, row in enumerate(pieces)
    ]


def group(refs, count, size):
    return [refs[i * size : (i + 1) * size] for i in range(count)]


def hidden_kernel(planes, m, second, base_ref, *refs):
    tokens, refs = group(refs, 4, m), refs[4 * m :]
    weights, refs = group(refs, planes, 2), refs[2 * planes :]
    if second:
        rect, out, wv, tv, rv, ov, wsem, tsem, rsem, osem = refs
        outs = [(out, ov)]
    else:
        act, rect, wv, tv, rv, ov, wsem, tsem, osem = refs
        outs = [(act, ov), (rect, rv)]
    rows = tokens[0][0].shape[0]
    width = wv.shape[0]
    wcopies = start(weight_copies(base_ref[0], weights, wv, wsem))
    tcopies = token_copies(tokens, tv, tsem)
    for row in tcopies:
        start(row)
    if second:
        rcopies = start([pltpu.make_async_copy(rect.at[p], rv.at[p], rsem.at[p]) for p in range(4)])
    wait(wcopies)
    tile = min(width, 256)
    ocopies = []
    for p in range(4):
        wait(tcopies[p])
        if second:
            rcopies[p].wait()

        @pl.loop(0, width // tile)
        def _(i):
            at = pl.ds(pl.multiple_of(i * tile, tile), tile)
            o = dot(wv[at, :], tv[pl.ds(p * rows, rows), :], NT)
            if second:
                ov[p, at, :] = (2.0 * rv[p, at, :].astype(F32) * o).astype(BF)
            else:
                r = jnp.maximum(o, 0.0)
                rv[p, at, :] = r.astype(BF)
                ov[p, at, :] = (r * r).astype(BF)

        for k, (dest, source) in enumerate(outs):
            ocopies += start(
                [pltpu.make_async_copy(source.at[p], dest.at[p], osem.at[p * len(outs) + k])]
            )
    wait(ocopies)


def grad_kernel(planes, m, scale, base_ref, *refs):
    tokens, refs = group(refs, 4, m), refs[4 * m :]
    hidden, *outs, av, tv, ov, tsem, asem, osem = refs
    rows = tokens[0][0].shape[0]
    width = av.shape[0]
    base = base_ref[0]
    acopies = start(
        [
            pltpu.make_async_copy(hidden.at[p], av.at[:, pl.ds(p * rows, rows)], asem.at[p])
            for p in range(4)
        ]
    )
    tcopies = token_copies(tokens, tv, tsem)
    for c in range(m):
        start([row[c] for row in tcopies])
    wait(acopies)
    tile = min(width, 512)
    even = (base & 1) == 0
    each = 2 * planes // m

    def out_copies(mz, ky):
        return [
            pltpu.make_async_copy(
                ov.at[mz, k, ky], outs[2 * mz + k].at[ky], osem.at[mz, k, ky]
            )
            for k in range(2)
        ]

    for c in range(m):
        wait([row[c] for row in tcopies])

        @pl.loop(c * each, (c + 1) * each)
        def _(q):
            mask = (base >> 1) ^ q
            mz, ky = mask >> 1, mask & 1
            cols = pl.ds(pl.multiple_of(q * 2 * LANES, 2 * LANES), 2 * LANES)

            @pl.loop(0, width // tile)
            def _(i):
                at = pl.ds(pl.multiple_of(i * tile, tile), tile)
                o = dot(av[at, :], tv[:, cols], NN) * scale
                lo, hi = o[:, :LANES], o[:, LANES:]
                ov[mz, 0, ky, at, :] = jnp.where(even, lo, hi).astype(BF)
                ov[mz, 1, ky, at, :] = jnp.where(even, hi, lo).astype(BF)

            for plane in range(planes):

                @pl.when(mz == plane)
                def _():
                    start(out_copies(plane, ky))

    for plane in range(planes):
        for ky in range(2):
            wait(out_copies(plane, ky))


def input_kernel(planes, m, base_ref, *refs):
    hidden, refs = refs[0], refs[1:]
    weights, refs = group(refs, planes, 2), refs[2 * planes :]
    outs, (wv, av, ov, wsem, asem, osem) = refs[: 4 * m], refs[4 * m :]
    part = outs[0].shape[1]
    wcopies = start(weight_copies(base_ref[0], weights, wv, wsem))
    acopies = start([pltpu.make_async_copy(hidden.at[p], av.at[p], asem.at[p]) for p in range(4)])
    wait(wcopies)
    wait(acopies)
    ocopies = []
    for c in range(m - 1, -1, -1):
        for p in range(3, -1, -1):
            ov[c, p] = dot(av[p], wv[:, c * part : (c + 1) * part], TN).astype(BF)
            k = c * 4 + p
            ocopies += start([pltpu.make_async_copy(ov.at[c, p], outs[k], osem.at[k])])
    wait(ocopies)


def per_device(x, dy, up, down):
    n, m = lax.axis_size("fs"), lax.axis_size("tp")
    rows, part = x.shape
    d_rows, ff = up.shape
    planes = n // 4
    if d_rows != LANES or planes < m:
        return plain(x, dy, up, down)
    f, t = lax.axis_index("fs"), lax.axis_index("tp")
    py, zl = (f // 2) % 2, (f // 4) % 2
    base = (f ^ (4 * t * (planes // m))).astype(jnp.int32).reshape(1)
    width = ff // 4
    scale = float(rows * n) ** -0.5
    flops = 2 * 4 * rows * width * n * d_rows

    def send(value, mask, core=0):
        perm = [(i * m + c, (i ^ mask) * m + (c ^ core)) for i in range(n) for c in range(m)]
        return lax.ppermute(value, AXES, perm)

    def gather_tokens(value):
        near = send(value, 4)
        side = send(value, 2)
        pieces = (value, side, near, send(near, 2))
        return [[p] + [send(p, 0, c) for c in range(1, m)] for p in pieces]

    def gather_weights(tag, w):
        def half(y):
            if tag == "u":
                return pick(w.reshape(d_rows, 2, ff // 2), 1, y).T.reshape(2, width, d_rows)
            return pick(w.reshape(2, 2, width, d_rows), 0, y)

        theirs = send(half(1 - py), 2)
        mine = half(py)
        both = jnp.stack([mine, theirs])
        halves = [pick(both, 1, zl), pick(both, 1, 1 - zl)]
        pieces = []
        for mz in range(planes):
            piece = send(halves[mz % 2], 4 * mz) if mz else halves[0]
            pieces.append([piece, send(piece, 1)])
        return pieces

    def flat(lists):
        return [a for row in lists for a in row]

    x4 = gather_tokens(x)
    wu = gather_weights("u", up)
    dy4 = gather_tokens(dy)
    wd = gather_weights("d", down)
    every = 4 * rows
    hid, feats = (4, width, rows), n * d_rows
    nw, nt = 4 * planes, 4 * m

    act, rect = call(
        functools.partial(hidden_kernel, planes, m, False),
        [hid, hid],
        [(width, feats), (every, feats), hid, hid],
        [nw, nt, 8],
        flops,
        [base, *flat(x4), *flat(wu)],
    )

    def grad(tokens, hidden):
        return call(
            functools.partial(grad_kernel, planes, m, scale),
            [(2, width, LANES)] * (2 * planes),
            [(width, every), (every, feats), (planes, 2, 2, width, LANES)],
            [nt, 4, (planes, 2, 2)],
            flops,
            [base, *flat(tokens), hidden],
        )

    def scatter(parts):
        total = [None, None]
        for mz in reversed(range(planes)):
            got = send(parts[2 * mz + 1], 1).astype(F32)
            value = parts[2 * mz].astype(F32) + got
            if mz:
                value = value.astype(BF)
            if mz:
                value = send(value, 4 * mz).astype(F32)
            b = mz % 2
            total[b] = value if total[b] is None else total[b] + value
        other = send(jnp.stack([total[0][1], total[1][1]]).astype(BF), 2)
        a, b = total[0][0], total[1][0]
        c, d = other[0].astype(F32), other[1].astype(F32)
        a, b = jnp.where(zl == 0, a, b), jnp.where(zl == 0, b, a)
        c, d = jnp.where(zl == 0, c, d), jnp.where(zl == 0, d, c)
        a, b, c, d = (
            jnp.where(py == 0, a, c),
            jnp.where(py == 0, b, d),
            jnp.where(py == 0, c, a),
            jnp.where(py == 0, d, b),
        )
        return jnp.concatenate([a, b, c, d])

    down_grad = scatter(grad(dy4, act))
    (pre_grad,) = call(
        functools.partial(hidden_kernel, planes, m, True),
        [hid],
        [(width, feats), (every, feats), hid, hid],
        [nw, nt, 4, 4],
        flops,
        [base, *flat(dy4), *flat(wd), rect],
    )
    up_grad = scatter(grad(x4, pre_grad)).T
    dx = call(
        functools.partial(input_kernel, planes, m),
        [(rows, part)] * (4 * m),
        [(width, feats), hid, (m, 4, rows, part)],
        [nw, 4, 4 * m],
        flops,
        [base, pre_grad, *flat(wu)],
    )
    own = [None] * 4
    for p in range(3, -1, -1):
        own[p] = dx[p].astype(F32)
        for c in range(1, m):
            own[p] = own[p] + send(dx[4 * c + p], 0, c).astype(F32)
    far = own[2] + send(own[3].astype(BF), 2).astype(F32)
    near = own[0] + send(own[1].astype(BF), 2).astype(F32)
    far = send(far.astype(BF), 4)
    input_grad = (near + far.astype(F32)).astype(BF)
    return input_grad, up_grad, down_grad


def solution(mesh):
    in_specs = (P("fs", "tp"), P("fs", "tp"), P("fs", "tp"), P("tp", "fs"))
    out_specs = (P("fs", "tp"), P("fs", "tp"), P("tp", "fs"))

    return jax.shard_map(
        per_device, mesh=mesh, in_specs=in_specs, out_specs=out_specs, check_vma=False
    )
```
